32 devices in a mesh: grp: 2 (over y), sp: 4 (over z), tp: 4 (over x, core).
Axes of the slice: x: 2, y: 2, z: 4, core: 2. Of those that a mesh axis runs over, the one named last changes fastest.
Arguments:
- query_latent: bfloat16 [1024, 768], P(('grp', 'sp')), parts along dimension 0, may hold values from -6 to 6
- key_latent: bfloat16 [1024, 256], P(('grp', 'sp', 'tp')), parts along dimension 0, may hold values from -20 to 20
- rotary_key: bfloat16 [1024, 64], P(('grp', 'sp', 'tp')), parts along dimension 0, may hold values from -1000 to 1000
- query_gain: float32 [768], replicated, may hold values from 0.1 to 1.9
- latent_gain: float32 [256], replicated, may hold values from 0.1 to 1.9
- query_up: bfloat16 [768, 3072], P(None, 'tp'), may hold values from -0.21875 to 0.21875
- key_up: bfloat16 [256, 2048], P(None, 'tp'), may hold values from -0.375 to 0.375
- value_up: bfloat16 [256, 2048], P(None, 'tp'), may hold values from -0.375 to 0.375
- out_gain: float32 [2048], P('tp'), may hold values from 0.1 to 1.9
- out_weight: bfloat16 [2048, 4096], P('sp', 'tp'), may hold values from -0.125 to 0.125
Outputs:
- mixed: bfloat16 [1024, 4096], P(('grp', 'sp'), 'tp'), parts along dimension 0
The draws below stay inside these ranges and needn't reach their ends.
There are 2 independent parts, one for each index of `grp`. The reference program is written for one: setup_inputs(seed, part) draws one part's arguments, and reference() takes and returns one part's arrays. A program takes and returns all parts, laid end to end along the dimension named above; an argument that names none is the same for every part. Nothing has to cross between parts.
All inputs are finite; a program needn't handle non-finite values.
Results may differ from the reference program's by a relative error of at most 0.02.
The reference program's roundings to bfloat16 on the way count: a program that leaves them out, or rounds other values in their place, can miss the bound.
Values may be sent and summed in bfloat16 or wider, within the bound.
A program may use at most 128 MiB of HBM per device.

```python
import jax
import jax.numpy as jnp
from jax import lax

D_MODEL = 4096
HEADS = 16
NOPE_DIM = 128
ROPE_DIM = 64
VALUE_DIM = 128
QRANK = 768
KVRANK = 256
TOK_DEV = 128
TOKENS = 512
N_SP = 4


def draw_key_latent(key, part):
    first_key, second_key = jax.random.split(jax.random.fold_in(key, 11), 2)
    blocks = TOKENS // TOK_DEV
    offsets = jax.random.normal(second_key, (blocks, KVRANK), jnp.float32)
    noise = jax.random.normal(first_key, (TOKENS, KVRANK), jnp.float32)
    offset_rows = jnp.repeat(offsets, TOK_DEV, axis=0)
    return jnp.clip(noise + offset_rows, -20.0, 20.0).astype(jnp.bfloat16)


def draw_rotary_key(key, part):
    first_key = jax.random.fold_in(jax.random.fold_in(key, 23), 0)
    values = jax.random.normal(first_key, (TOKENS, ROPE_DIM), jnp.float32)
    return jnp.clip(values, -1000.0, 1000.0).astype(jnp.bfloat16)


def shard_levels(rng, extent, cuts, smallest, top_value):
    def one(dim, shards_of):
        heights = jax.random.uniform(jax.random.fold_in(jax.random.fold_in(rng, 6), dim), (shards_of,), jnp.float32, smallest / len(cuts), top_value / len(cuts))
        return jnp.repeat(jnp.exp(heights), extent[dim] // shards_of).reshape((-1,) + (1,) * (len(extent) - dim - 1))

    factor_of = one(*cuts[0])
    for cut in cuts[1:]:
        factor_of = factor_of * one(*cut)
    return factor_of


def scatter_about(own_key, extent, scale, reach, pieces=(), kind=jnp.bfloat16):
    result = jax.random.normal(own_key, extent, jnp.float32) * scale
    if len(pieces) > 0:
        result = shard_levels(own_key, extent, pieces, -0.22, 0.18) * result
    return jnp.clip(result, min=-reach, max=reach).astype(kind)


def setup_inputs(seed: int = 0, part: int = 0) -> dict:
    keys = jax.random.split(jax.random.key(seed), 11)
    own_keys = jax.random.split(jax.random.fold_in(keys[10], part), 11)
    return {
        "query_latent": scatter_about(own_keys[0], (TOKENS, QRANK), 1.0, 6.0, ((0, 4),)),
        "key_latent": draw_key_latent(jax.random.fold_in(jax.random.fold_in(keys[10], part), 71), part),
        "rotary_key": draw_rotary_key(jax.random.fold_in(jax.random.fold_in(keys[10], part), 71), part),
        "query_gain": jnp.clip(1.0 + 0.18 * jax.random.normal(keys[3], (QRANK,), jnp.float32), 0.1, 1.9),
        "latent_gain": jnp.clip(1.0 + 0.18 * jax.random.normal(keys[4], (KVRANK,), jnp.float32), 0.1, 1.9),
        "query_up": scatter_about(keys[5], (QRANK, HEADS * (NOPE_DIM + ROPE_DIM)), QRANK ** -0.5, 0.21875, ((1, 4),)),
        "key_up": scatter_about(keys[6], (KVRANK, HEADS * NOPE_DIM), KVRANK ** -0.5, 0.375, ((1, 4),)),
        "value_up": scatter_about(keys[7], (KVRANK, HEADS * VALUE_DIM), KVRANK ** -0.5, 0.375, ((1, 4),)),
        "out_gain": jnp.clip(1.0 + 0.18 * jax.random.normal(keys[8], (HEADS * VALUE_DIM,), jnp.float32), 0.1, 1.9),
        "out_weight": scatter_about(keys[9], (HEADS * VALUE_DIM, D_MODEL), (HEADS * VALUE_DIM) ** -0.5, 0.125, ((0, 4), (1, 4))),
    }


norm_eps = 1e-06
rope_theta = 10000.0

def rms_scaled(inputs, gain_vec):
    widened = inputs.astype(jnp.float32)
    return widened * lax.rsqrt(lax.optimization_barrier(jnp.mean(widened * widened, axis=-1, keepdims=True)) + norm_eps) * gain_vec

def rotate_half(inputs, positions):
    half_width = inputs.shape[-1] // 2
    inverse = rope_theta ** (-jnp.arange(half_width, dtype=jnp.float32) / half_width)
    angles = positions[:, None] * inverse[None, :]
    if inputs.ndim == 3:
        angles = angles[:, None, :]
    cosine = jnp.cos(angles)
    sine = jnp.sin(angles)
    widened = inputs.astype(jnp.float32)
    first = widened[..., :half_width]
    second = widened[..., half_width:]
    return jnp.concatenate([first * cosine - second * sine, second * cosine + first * sine], axis=-1)

def reference(query_latent, key_latent, rotary_key, query_gain, latent_gain, query_up, key_up, value_up, out_gain, out_weight):
    positions = jnp.arange(TOKENS, dtype=jnp.float32)
    score_scale = (NOPE_DIM + ROPE_DIM) ** (-0.5)
    query_normed = rms_scaled(query_latent, query_gain).astype(jnp.bfloat16)
    query_full = jnp.dot(query_normed, query_up, preferred_element_type=jnp.float32).astype(jnp.bfloat16)
    query_full = query_full.reshape(TOKENS, HEADS, NOPE_DIM + ROPE_DIM)
    query_plain = query_full[..., :NOPE_DIM]
    query_turned = rotate_half(query_full[..., NOPE_DIM:], positions).astype(jnp.bfloat16)
    latent_normed = rms_scaled(key_latent, latent_gain).astype(jnp.bfloat16)
    key_turned = rotate_half(rotary_key, positions).astype(jnp.bfloat16)
    key_plain = jnp.dot(latent_normed, key_up, preferred_element_type=jnp.float32).astype(jnp.bfloat16)
    key_wide = key_plain.reshape(TOKENS, HEADS, NOPE_DIM).astype(jnp.float32)
    turned_wide = key_turned.astype(jnp.float32)
    latent_wide = latent_normed.astype(jnp.float32)
    value_heads = value_up.astype(jnp.float32).reshape(KVRANK, HEADS, VALUE_DIM)

    def one_block(block_index):
        begin = (block_index * TOK_DEV).astype(jnp.int32)
        plain = lax.dynamic_slice_in_dim(query_plain, begin, TOK_DEV, 0).astype(jnp.float32)
        turned = lax.dynamic_slice_in_dim(query_turned, begin, TOK_DEV, 0).astype(jnp.float32)
        scores = jnp.einsum('qhd,khd->qhk', plain, key_wide) + jnp.einsum('qhd,kd->qhk', turned, turned_wide)
        scores = scores * score_scale
        row_top = lax.optimization_barrier(jnp.max(scores, axis=-1, keepdims=True))
        expo = jnp.exp(scores - row_top)
        total = lax.optimization_barrier(jnp.sum(expo, axis=-1))
        weights = lax.optimization_barrier(expo.astype(jnp.bfloat16)).astype(jnp.float32)
        latent_mix = jnp.einsum('qhk,kc->qhc', weights, latent_wide) / total[..., None]
        latent_mix = lax.optimization_barrier(latent_mix.astype(jnp.bfloat16)).astype(jnp.float32)
        head_out = jnp.einsum('qhc,chd->qhd', latent_mix, value_heads).astype(jnp.bfloat16)
        return head_out.reshape(TOK_DEV, HEADS * VALUE_DIM)
    head_out = lax.map(one_block, jnp.arange(N_SP, dtype=jnp.int32)).reshape(TOKENS, HEADS * VALUE_DIM)
    widened = head_out.astype(jnp.float32)
    mean_square = lax.optimization_barrier(jnp.mean(widened * widened, axis=1))
    gained = (widened * out_gain).astype(jnp.bfloat16)
    projected = jnp.dot(gained, out_weight, preferred_element_type=jnp.float32)
    return (projected * lax.rsqrt(mean_square + norm_eps)[:, None]).astype(jnp.bfloat16)
```

```python
import functools

import jax
import jax.numpy as jnp
import numpy as np
from jax import lax
from jax.experimental import pallas as pl
from jax.experimental.pallas import tpu as pltpu
from jax.sharding import PartitionSpec as P

HEADS = 16
NOPE_DIM = 128
ROPE_DIM = 64
VALUE_DIM = 128
KVRANK = 256


norm_eps = 1e-06
rope_theta = 10000.0


def rms_scaled(inputs, gain_vec):
    widened = inputs.astype(jnp.float32)
    return (
        widened
        * lax.rsqrt(jnp.mean(widened * widened, axis=-1, keepdims=True) + norm_eps)
        * gain_vec
    )


def rotate_half(inputs, positions):
    half_width = inputs.shape[-1] // 2
    inverse = rope_theta ** (-jnp.arange(half_width, dtype=jnp.float32) / half_width)
    angles = positions[:, None] * inverse[None, :]
    if inputs.ndim == 3:
        angles = angles[:, None, :]
    cosine = jnp.cos(angles)
    sine = jnp.sin(angles)
    widened = inputs.astype(jnp.float32)
    first = widened[..., :half_width]
    second = widened[..., half_width:]
    return jnp.concatenate(
        [first * cosine - second * sine, second * cosine + first * sine], axis=-1
    )


def on_device(
    query_latent,
    key_latent,
    rotary_key,
    query_gain,
    latent_gain,
    query_up,
    key_up,
    value_up,
    out_gain,
    out_weight,
):
    block_rows = query_latent.shape[0]
    row_count = key_latent.shape[0]
    head_local = key_up.shape[1] // NOPE_DIM
    block_start = lax.axis_index("sp") * block_rows
    own_start = block_start + lax.axis_index("tp") * row_count
    score_scale = (NOPE_DIM + ROPE_DIM) ** (-0.5)
    normed = rms_scaled(query_latent, query_gain).astype(jnp.bfloat16)
    query_full = jnp.dot(normed, query_up, preferred_element_type=jnp.float32).astype(jnp.bfloat16)
    query_full = query_full.reshape(block_rows, head_local, NOPE_DIM + ROPE_DIM)
    query_positions = (block_start + jnp.arange(block_rows, dtype=jnp.int32)).astype(jnp.float32)
    query_plain = query_full[..., :NOPE_DIM]
    query_turned = rotate_half(query_full[..., NOPE_DIM:], query_positions).astype(jnp.bfloat16)
    latent_normed = rms_scaled(key_latent, latent_gain).astype(jnp.bfloat16)
    own_positions = (own_start + jnp.arange(row_count, dtype=jnp.int32)).astype(jnp.float32)
    key_turned = rotate_half(rotary_key, own_positions).astype(jnp.bfloat16)
    running_max = jnp.full((block_rows, head_local), -1e30, jnp.float32)
    running_sum = jnp.zeros((block_rows, head_local), jnp.float32)
    weighted = jnp.zeros((block_rows, head_local, KVRANK), jnp.float32)
    latents = lax.all_gather(latent_normed, ("sp", "tp"), axis=0, tiled=True)
    turned_keys = lax.all_gather(key_turned, ("sp", "tp"), axis=0, tiled=True)
    portion_rows = latents.shape[0]
    step_rows = min(portion_rows, 2048)
    for begin in range(0, portion_rows, step_rows):
        latent_part = latents[begin : begin + step_rows]
        turned_part = turned_keys[begin : begin + step_rows]
        key_plain = jnp.dot(latent_part, key_up, preferred_element_type=jnp.float32).astype(
            jnp.bfloat16
        )
        key_plain = key_plain.reshape(latent_part.shape[0], head_local, NOPE_DIM)
        scores = jnp.einsum(
            "qhd,khd->qhk", query_plain, key_plain, preferred_element_type=jnp.float32
        )
        scores = scores + jnp.einsum(
            "qhd,kd->qhk", query_turned, turned_part, preferred_element_type=jnp.float32
        )
        scores = scores * score_scale
        new_max = jnp.maximum(running_max, jnp.max(scores, axis=-1))
        rescale = jnp.exp(running_max - new_max)
        expo = jnp.exp(scores - new_max[..., None])
        running_sum = running_sum * rescale + jnp.sum(expo, axis=-1)
        weighted = weighted * rescale[..., None] + jnp.einsum(
            "qhk,kc->qhc",
            expo.astype(jnp.bfloat16),
            latent_part,
            preferred_element_type=jnp.float32,
        )
        running_max = new_max
    final_state = (running_max, running_sum, weighted)
    running_max, running_sum, weighted = final_state
    latent_mix = (weighted / running_sum[..., None]).astype(jnp.bfloat16)
    value_heads = value_up.reshape(KVRANK, head_local, VALUE_DIM)
    head_out = jnp.einsum(
        "qhc,chd->qhd", latent_mix, value_heads, preferred_element_type=jnp.float32
    ).astype(jnp.bfloat16)
    head_out = head_out.reshape(block_rows, head_local * VALUE_DIM)
    widened = head_out.astype(jnp.float32)
    square_part = jnp.sum(widened * widened, axis=1)
    gained = (widened * out_gain).astype(jnp.bfloat16)
    all_gained, square_parts = (
        lax.all_gather(gained, "tp", axis=1, tiled=True),
        lax.all_gather(square_part[:, None].astype(jnp.bfloat16), "tp", axis=1, tiled=True).astype(
            jnp.float32
        ),
    )
    all_squares = jnp.sum(square_parts, axis=1)
    own_sums = jnp.dot(
        all_gained,
        lax.all_gather(out_weight, "sp", axis=0, tiled=True),
        preferred_element_type=jnp.float32,
    )
    mean_square = all_squares / (HEADS * VALUE_DIM)
    return (own_sums * lax.rsqrt(mean_square + norm_eps)[:, None]).astype(jnp.bfloat16)


CHUNKS = 4
MOST_STEPS = 8


def rope_table(tokens, width):
    half = width // 2
    inverse = np.float32(rope_theta) ** (-np.arange(half, dtype=np.float32) / np.float32(half))
    angles = np.arange(tokens, dtype=np.float32)[:, None] * inverse.astype(np.float32)[None, :]
    wide = angles.astype(np.float32).astype(np.float64)
    cosine, sine = np.cos(wide), np.sin(wide)
    return np.concatenate([cosine, cosine, -sine, sine], axis=1).astype(np.float32)


def turned(wide, table):
    width = wide.shape[-1]
    half = width // 2
    swapped = jnp.concatenate([wide[:, half:], wide[:, :half]], axis=1)
    return wide * table[:, :width] + swapped * table[:, width:]


def kernel(
    n_sp, n_tp,
    ql, kl, rk, qg, lg, og, table, qup, kup, vup, ow, out,
    lat, rot, wbuf, qbuf, kbuf, vbuf, latn, kturn, qfull, qnorm, gall, acc,
    local, s1_send, s1_recv, s2_send, s2_recv, g_send, g_recv,
    w_send, w_recv, y_send, y_recv,
):
    z, t, g = lax.axis_index("sp"), lax.axis_index("tp"), lax.axis_index("grp")
    parity = lax.rem(g, 2)
    partner = g + 1 - 2 * parity
    block_rows = ql.shape[0]
    depth = ow.shape[0]
    half = depth // 2
    piece = half // CHUNKS
    heads = kup.shape[1] // NOPE_DIM
    cols = heads * VALUE_DIM
    head_width = NOPE_DIM + ROPE_DIM
    keys = n_sp * n_tp * kl.shape[0]

    near = pl.ds(pl.multiple_of(parity * half, half), half)
    far = pl.ds(pl.multiple_of((1 - parity) * half, half), half)
    loads = [
        pltpu.make_async_copy(ow.at[near], wbuf.at[z, near], local.at[0]),
        pltpu.make_async_copy(kl, lat.at[z, t], local.at[1]),
        pltpu.make_async_copy(rk, rot.at[z, t], local.at[2]),
        pltpu.make_async_copy(qup, qbuf, local.at[3]),
        pltpu.make_async_copy(kup, kbuf, local.at[4]),
        pltpu.make_async_copy(vup, vbuf, local.at[5]),
        pltpu.make_async_copy(ow.at[far], wbuf.at[z, far], local.at[6]),
    ]
    for load in loads:
        load.start()

    barrier = pltpu.get_barrier_semaphore()
    for d in range(1, n_sp):
        pl.semaphore_signal(barrier, inc=1, device_id={"sp": lax.rem(z + d, n_sp)}, device_id_type=MESH)
    for d in range(1, n_tp):
        pl.semaphore_signal(barrier, inc=1, device_id={"tp": lax.rem(t + d, n_tp)}, device_id_type=MESH)
    pl.semaphore_signal(barrier, inc=1, device_id={"grp": partner}, device_id_type=MESH)
    pl.semaphore_wait(barrier, n_sp + n_tp - 1)

    def remote(src, dst, send, recv, target):
        return pltpu.make_async_remote_copy(
            src_ref=src, dst_ref=dst, send_sem=send, recv_sem=recv,
            device_id=target, device_id_type=MESH,
        )

    first = []
    for d in range(1, n_sp):
        target = {"sp": lax.rem(z + d, n_sp)}
        first.append(remote(kl, lat.at[z, t], s1_send.at[0, d], s1_recv.at[0, d], target))
        first.append(remote(rk, rot.at[z, t], s1_send.at[1, d], s1_recv.at[1, d], target))
    for copy in first:
        copy.start()

    def rows_of(b, c):
        return wbuf.at[b, pl.ds(pl.multiple_of(parity * half + c * piece, piece), piece)]

    def far_rows_of(b, c):
        return wbuf.at[b, pl.ds(pl.multiple_of((1 - parity) * half + c * piece, piece), piece)]

    def along(b, c, up):
        return remote(
            rows_of(b, c), rows_of(b, c), w_send.at[up, b, c], w_recv.at[b, c],
            {"sp": z + 1 if up else z - 1},
        )

    def across(b, c):
        return remote(rows_of(b, c), rows_of(b, c), y_send.at[b, c], y_recv.at[b, c], {"grp": partner})

    has_up, has_down = z < n_sp - 1, z > 0
    loads[0].wait()
    for c in range(CHUNKS):
        @pl.when(has_up)
        def _():
            along(z, c, 1).start()

        @pl.when(has_down)
        def _():
            along(z, c, 0).start()

    def event(k, c):
        @pl.when(z >= k)
        def _():
            b = z - k
            along(b, c, 1).wait_recv()

            @pl.when(has_up)
            def _():
                along(b, c, 1).start()

            across(b, c).start()

        @pl.when(z + k < n_sp)
        def _():
            b = z + k
            along(b, c, 0).wait_recv()

            @pl.when(has_down)
            def _():
                along(b, c, 0).start()

            across(b, c).start()

    def block_product(b):
        acc[...] += jnp.dot(gall[b, :, :cols], wbuf[b], preferred_element_type=jnp.float32)

    def finish(k):
        @pl.when(z >= k)
        def _():
            for c in range(CHUNKS):
                across(z - k, c).wait_recv()
            block_product(z - k)

        @pl.when(z + k < n_sp)
        def _():
            for c in range(CHUNKS):
                across(z + k, c).wait_recv()
            block_product(z + k)

    second = []
    for d in range(1, n_tp):
        target = {"tp": lax.rem(t + d, n_tp)}
        second.append(remote(lat.at[:, t], lat.at[:, t], s2_send.at[0, d], s2_recv.at[0, d], target))
        second.append(remote(rot.at[:, t], rot.at[:, t], s2_send.at[1, d], s2_recv.at[1, d], target))

    def queries():
        wide = ql[...].astype(jnp.float32)
        mean = jnp.mean(wide * wide, axis=-1, keepdims=True)
        qnorm[...] = (wide * lax.rsqrt(mean + norm_eps) * qg[...]).astype(jnp.bfloat16)
        loads[3].wait()
        qfull[...] = jnp.dot(qnorm[...], qbuf[...], preferred_element_type=jnp.float32).astype(
            jnp.bfloat16
        )

    def spread():
        loads[1].wait()
        loads[2].wait()
        for copy in first:
            copy.wait_recv()
        for copy in second:
            copy.start()

    def latents():
        for copy in second:
            copy.wait_recv()
        wide = lat[...].reshape(keys, lat.shape[-1]).astype(jnp.float32)
        mean = jnp.mean(wide * wide, axis=-1, keepdims=True)
        latn[...] = (wide * lax.rsqrt(mean + norm_eps) * lg[...]).astype(jnp.bfloat16)
        spun = rot[...].reshape(keys, rot.shape[-1]).astype(jnp.float32)
        kturn[...] = turned(spun, table[...]).astype(jnp.bfloat16)
        loads[4].wait()
        loads[5].wait()

    transposed = (((1,), (1,)), ((), ()))

    def attend(h):
        start = h * head_width
        plain = qfull[:, start : start + NOPE_DIM]
        spun = qfull[:, start + NOPE_DIM : start + head_width].astype(jnp.float32)
        own = table[pl.ds(pl.multiple_of(z * block_rows, block_rows), block_rows), :]
        spun = turned(spun, own).astype(jnp.bfloat16)
        key_plain = jnp.dot(
            latn[...], kbuf[:, h * NOPE_DIM : (h + 1) * NOPE_DIM], preferred_element_type=jnp.float32
        ).astype(jnp.bfloat16)
        scores = lax.dot_general(plain, key_plain, transposed, preferred_element_type=jnp.float32)
        scores = scores + lax.dot_general(
            spun, kturn[...], transposed, preferred_element_type=jnp.float32
        )
        scores = scores * (head_width ** (-0.5))
        expo = jnp.exp(scores - jnp.max(scores, axis=-1, keepdims=True))
        total = jnp.sum(expo, axis=-1, keepdims=True)
        mix = jnp.dot(expo.astype(jnp.bfloat16), latn[...], preferred_element_type=jnp.float32)
        mix = (mix / total).astype(jnp.bfloat16)
        head_out = jnp.dot(
            mix, vbuf[:, h * VALUE_DIM : (h + 1) * VALUE_DIM], preferred_element_type=jnp.float32
        ).astype(jnp.bfloat16)
        wide = head_out.astype(jnp.float32)
        gained = wide * og[:, h * VALUE_DIM : (h + 1) * VALUE_DIM]
        gall[t, :, h * VALUE_DIM : (h + 1) * VALUE_DIM] = gained.astype(jnp.bfloat16)
        square = jnp.sum(wide * wide, axis=-1, keepdims=True)
        if h:
            square = square + acc[:, :1]
        acc[:, :VALUE_DIM] = jnp.broadcast_to(square, (block_rows, VALUE_DIM))
        if h == heads - 1:
            gall[t, :, cols:] = acc[:, :VALUE_DIM].astype(jnp.bfloat16)

    shares = [
        remote(gall.at[t], gall.at[t], g_send.at[d], g_recv.at[d], {"tp": lax.rem(t + d, n_tp)})
        for d in range(1, n_tp)
    ]

    def share():
        for copy in shares:
            copy.start()

    def own_product():
        for copy in shares:
            copy.wait_recv()
        loads[6].wait()
        acc[...] = jnp.zeros_like(acc)
        block_product(z)

    attends = [functools.partial(attend, h) for h in range(heads)]
    split = (heads + 1) // 2
    tasks = {
        0: [queries, spread],
        1: [latents] + attends[:1],
        2: attends[1 : split + 1],
        3: attends[split + 1 :],
        4: [share],
        5: [],
        6: [own_product],
    }
    slot = 0
    for k in range(1, n_sp):
        for c in range(CHUNKS):
            for task in tasks.pop(slot, []):
                task()
            event(k, c)
            slot += 1
        if k > 2:
            finish(k - 2)
    for left in sorted(tasks):
        for task in tasks[left]:
            task()
    for k in range(max(n_sp - 2, 1), n_sp):
        finish(k)

    squares = gall[0, :, cols : cols + 1].astype(jnp.float32)
    for p in range(1, n_tp):
        squares = squares + gall[p, :, cols : cols + 1].astype(jnp.float32)
    scale = lax.rsqrt(squares / (n_tp * cols) + norm_eps)
    out[...] = (acc[...] * scale).astype(out.dtype)

    for copy in first + second + shares:
        copy.wait_send()
    for c in range(CHUNKS):
        @pl.when(has_up)
        def _():
            along(z, c, 1).wait_send()

        @pl.when(has_down)
        def _():
            along(z, c, 0).wait_send()

    for k in range(1, n_sp):
        for c in range(CHUNKS):
            @pl.when(z >= k)
            def _():
                across(z - k, c).wait_send()

            @pl.when(jnp.logical_and(z >= k, has_up))
            def _():
                along(z - k, c, 1).wait_send()

            @pl.when(z + k < n_sp)
            def _():
                across(z + k, c).wait_send()

            @pl.when(jnp.logical_and(z + k < n_sp, has_down))
            def _():
                along(z + k, c, 0).wait_send()


MESH = pl.DeviceIdType.MESH


def on_device_fused(
    n_sp, n_tp,
    query_latent, key_latent, rotary_key, query_gain, latent_gain,
    query_up, key_up, value_up, out_gain, out_weight,
):
    block_rows, row_count = query_latent.shape[0], key_latent.shape[0]
    rank, width = key_latent.shape[1], rotary_key.shape[1]
    keys = n_sp * n_tp * row_count
    depth, features = out_weight.shape
    cols = value_up.shape[1]
    vmem, bf16, dma = pltpu.VMEM, jnp.bfloat16, pltpu.SemaphoreType.DMA
    table = jnp.asarray(rope_table(keys, width))
    in_vmem = pl.BlockSpec(memory_space=pltpu.VMEM)
    in_hbm = pl.BlockSpec(memory_space=pl.ANY)
    return pl.pallas_call(
        functools.partial(kernel, n_sp, n_tp),
        out_shape=jax.ShapeDtypeStruct((block_rows, features), bf16),
        in_specs=[in_vmem] * 7 + [in_hbm] * 4,
        out_specs=in_vmem,
        scratch_shapes=[
            vmem((n_sp, n_tp, row_count, rank), bf16),
            vmem((n_sp, n_tp, row_count, width), bf16),
            vmem((n_sp, depth, features), bf16),
            vmem(query_up.shape, bf16),
            vmem(key_up.shape, bf16),
            vmem(value_up.shape, bf16),
            vmem((keys, rank), bf16),
            vmem((keys, width), bf16),
            vmem((block_rows, query_up.shape[1]), bf16),
            vmem(query_latent.shape, bf16),
            vmem((n_tp, block_rows, cols + VALUE_DIM), bf16),
            vmem((block_rows, features), jnp.float32),
            dma((7,)),
            dma((2, n_sp)),
            dma((2, n_sp)),
            dma((2, n_tp)),
            dma((2, n_tp)),
            dma((n_tp,)),
            dma((n_tp,)),
            dma((2, n_sp, CHUNKS)),
            dma((n_sp, CHUNKS)),
            dma((n_sp, CHUNKS)),
            dma((n_sp, CHUNKS)),
        ],
        compiler_params=pltpu.CompilerParams(
            collective_id=0, has_side_effects=True, vmem_limit_bytes=48 * 1024 * 1024
        ),
    )(
        query_latent, key_latent, rotary_key, query_gain[None], latent_gain[None], out_gain[None],
        table, query_up, key_up, value_up, out_weight,
    )


def fits_fused(mesh):
    n_grp, n_sp, n_tp = (mesh.shape[name] for name in ("grp", "sp", "tp"))
    return n_grp % 2 == 0 and 1 < n_sp <= MOST_STEPS and n_sp == n_tp


def solution(mesh):
    in_specs = (
        P(("grp", "sp"), None),
        P(("grp", "sp", "tp"), None),
        P(("grp", "sp", "tp"), None),
        P(),
        P(),
        P(None, "tp"),
        P(None, "tp"),
        P(None, "tp"),
        P("tp"),
        P("sp", "tp"),
    )
    out_specs = P(("grp", "sp"), "tp")
    step = on_device
    if fits_fused(mesh):
        step = functools.partial(on_device_fused, mesh.shape["sp"], mesh.shape["tp"])
    return jax.shard_map(
        step, mesh=mesh, in_specs=in_specs, out_specs=out_specs, check_vma=False
    )
```

```python
import functools

import jax
import jax.numpy as jnp
import numpy as np
from jax import lax
from jax.experimental import pallas as pl
from jax.experimental.pallas import tpu as pltpu
from jax.sharding import PartitionSpec as P

HEADS = 16
NOPE_DIM = 128
ROPE_DIM = 64
VALUE_DIM = 128
KVRANK = 256


norm_eps = 1e-06
rope_theta = 10000.0


def rms_scaled(inputs, gain_vec):
    widened = inputs.astype(jnp.float32)
    return (
        widened
        * lax.rsqrt(jnp.mean(widened * widened, axis=-1, keepdims=True) + norm_eps)
        * gain_vec
    )


def rotate_half(inputs, positions):
    half_width = inputs.shape[-1] // 2
    inverse = rope_theta ** (-jnp.arange(half_width, dtype=jnp.float32) / half_width)
    angles = positions[:, None] * inverse[None, :]
    if inputs.ndim == 3:
        angles = angles[:, None, :]
    cosine = jnp.cos(angles)
    sine = jnp.sin(angles)
    widened = inputs.astype(jnp.float32)
    first = widened[..., :half_width]
    second = widened[..., half_width:]
    return jnp.concatenate(
        [first * cosine - second * sine, second * cosine + first * sine], axis=-1
    )


def on_device(
    query_latent,
    key_latent,
    rotary_key,
    query_gain,
    latent_gain,
    query_up,
    key_up,
    value_up,
    out_gain,
    out_weight,
):
    block_rows = query_latent.shape[0]
    row_count = key_latent.shape[0]
    head_local = key_up.shape[1] // NOPE_DIM
    block_start = lax.axis_index("sp") * block_rows
    own_start = block_start + lax.axis_index("tp") * row_count
    score_scale = (NOPE_DIM + ROPE_DIM) ** (-0.5)
    normed = rms_scaled(query_latent, query_gain).astype(jnp.bfloat16)
    query_full = jnp.dot(normed, query_up, preferred_element_type=jnp.float32).astype(jnp.bfloat16)
    query_full = query_full.reshape(block_rows, head_local, NOPE_DIM + ROPE_DIM)
    query_positions = (block_start + jnp.arange(block_rows, dtype=jnp.int32)).astype(jnp.float32)
    query_plain = query_full[..., :NOPE_DIM]
    query_turned = rotate_half(query_full[..., NOPE_DIM:], query_positions).astype(jnp.bfloat16)
    latent_normed = rms_scaled(key_latent, latent_gain).astype(jnp.bfloat16)
    own_positions = (own_start + jnp.arange(row_count, dtype=jnp.int32)).astype(jnp.float32)
    key_turned = rotate_half(rotary_key, own_positions).astype(jnp.bfloat16)
    running_max = jnp.full((block_rows, head_local), -1e30, jnp.float32)
    running_sum = jnp.zeros((block_rows, head_local), jnp.float32)
    weighted = jnp.zeros((block_rows, head_local, KVRANK), jnp.float32)
    latents = lax.all_gather(latent_normed, ("sp", "tp"), axis=0, tiled=True)
    turned_keys = lax.all_gather(key_turned, ("sp", "tp"), axis=0, tiled=True)
    portion_rows = latents.shape[0]
    step_rows = min(portion_rows, 2048)
    for begin in range(0, portion_rows, step_rows):
        latent_part = latents[begin : begin + step_rows]
        turned_part = turned_keys[begin : begin + step_rows]
        key_plain = jnp.dot(latent_part, key_up, preferred_element_type=jnp.float32).astype(
            jnp.bfloat16
        )
        key_plain = key_plain.reshape(latent_part.shape[0], head_local, NOPE_DIM)
        scores = jnp.einsum(
            "qhd,khd->qhk", query_plain, key_plain, preferred_element_type=jnp.float32
        )
        scores = scores + jnp.einsum(
            "qhd,kd->qhk", query_turned, turned_part, preferred_element_type=jnp.float32
        )
        scores = scores * score_scale
        new_max = jnp.maximum(running_max, jnp.max(scores, axis=-1))
        rescale = jnp.exp(running_max - new_max)
        expo = jnp.exp(scores - new_max[..., None])
        running_sum = running_sum * rescale + jnp.sum(expo, axis=-1)
        weighted = weighted * rescale[..., None] + jnp.einsum(
            "qhk,kc->qhc",
            expo.astype(jnp.bfloat16),
            latent_part,
            preferred_element_type=jnp.float32,
        )
        running_max = new_max
    final_state = (running_max, running_sum, weighted)
    running_max, running_sum, weighted = final_state
    latent_mix = (weighted / running_sum[..., None]).astype(jnp.bfloat16)
    value_heads = value_up.reshape(KVRANK, head_local, VALUE_DIM)
    head_out = jnp.einsum(
        "qhc,chd->qhd", latent_mix, value_heads, preferred_element_type=jnp.float32
    ).astype(jnp.bfloat16)
    head_out = head_out.reshape(block_rows, head_local * VALUE_DIM)
    widened = head_out.astype(jnp.float32)
    square_part = jnp.sum(widened * widened, axis=1)
    gained = (widened * out_gain).astype(jnp.bfloat16)
    all_gained, square_parts = (
        lax.all_gather(gained, "tp", axis=1, tiled=True),
        lax.all_gather(square_part[:, None].astype(jnp.bfloat16), "tp", axis=1, tiled=True).astype(
            jnp.float32
        ),
    )
    all_squares = jnp.sum(square_parts, axis=1)
    own_sums = jnp.dot(
        all_gained,
        lax.all_gather(out_weight, "sp", axis=0, tiled=True),
        preferred_element_type=jnp.float32,
    )
    mean_square = all_squares / (HEADS * VALUE_DIM)
    return (own_sums * lax.rsqrt(mean_square + norm_eps)[:, None]).astype(jnp.bfloat16)


CHUNKS = 4
LANES = 128
MOST_STEPS = 8


def rope_table(tokens, width):
    half = width // 2
    inverse = np.float32(rope_theta) ** (-np.arange(half, dtype=np.float32) / np.float32(half))
    angles = np.arange(tokens, dtype=np.float32)[:, None] * inverse.astype(np.float32)[None, :]
    wide = angles.astype(np.float32).astype(np.float64)
    cosine, sine = np.cos(wide), np.sin(wide)
    return np.concatenate([cosine, cosine, -sine, sine], axis=1).astype(np.float32)


def turned(wide, table):
    width = wide.shape[-1]
    half = width // 2
    swapped = jnp.concatenate([wide[:, half:], wide[:, :half]], axis=1)
    return wide * table[:, :width] + swapped * table[:, width:]


def kernel(
    n_sp, n_tp,
    ql_hbm, kl, rk, qg_hbm, lg_hbm, og_hbm, table_hbm, qup, kup, vup, ow, out,
    ql, qg, lg, og, table,
    lat, rot, wbuf, qbuf, kbuf, vbuf, latn, kturn, qfull, qnorm, gall, acc,
    far_gained, far_out, far_in,
    local, s1_send, s1_recv, s2_send, s2_recv, g_send, g_recv,
    w_send, w_recv, y_send, y_recv, f_send, f_recv,
):
    z, t, g = lax.axis_index("sp"), lax.axis_index("tp"), lax.axis_index("grp")
    parity = lax.rem(g, 2)
    partner = g + 1 - 2 * parity
    block_rows = ql.shape[0]
    depth = ow.shape[0]
    half = depth // 2
    piece = half // CHUNKS
    heads = kup.shape[1] // NOPE_DIM
    cols = heads * VALUE_DIM
    head_width = NOPE_DIM + ROPE_DIM
    keys = n_sp * n_tp * kl.shape[0]

    near = pl.ds(pl.multiple_of(parity * half, half), half)
    far_half = pl.ds(pl.multiple_of((1 - parity) * half, half), half)
    loads = [
        pltpu.make_async_copy(src, dst, local.at[i])
        for i, (src, dst) in enumerate((
            (kl, lat.at[z, t]),
            (rk, rot.at[z, t]),
            (ow.at[near], wbuf.at[z, near]),
            (ql_hbm, ql),
            (qg_hbm, qg),
            (qup, qbuf),
            (lg_hbm, lg),
            (table_hbm, table),
            (kup, kbuf),
            (vup, vbuf),
            (og_hbm, og),
            (ow.at[far_half], wbuf.at[z, far_half]),
        ))
    ]
    for load in loads:
        load.start()

    barrier = pltpu.get_barrier_semaphore()
    for d in range(1, n_sp):
        pl.semaphore_signal(barrier, inc=1, device_id={"sp": lax.rem(z + d, n_sp)}, device_id_type=MESH)
    for d in range(1, n_tp):
        pl.semaphore_signal(barrier, inc=1, device_id={"tp": lax.rem(t + d, n_tp)}, device_id_type=MESH)
    pl.semaphore_signal(barrier, inc=1, device_id={"grp": partner}, device_id_type=MESH)
    pl.semaphore_wait(barrier, n_sp + n_tp - 1)

    def remote(src, dst, send, recv, target):
        return pltpu.make_async_remote_copy(
            src_ref=src, dst_ref=dst, send_sem=send, recv_sem=recv,
            device_id=target, device_id_type=MESH,
        )

    first = []
    for d in range(1, n_sp):
        target = {"sp": lax.rem(z + d, n_sp)}
        first.append(remote(lat.at[z, t], lat.at[z, t], s1_send.at[0, d], s1_recv.at[0, d], target))
        first.append(remote(rot.at[z, t], rot.at[z, t], s1_send.at[1, d], s1_recv.at[1, d], target))
    loads[0].wait()
    loads[1].wait()
    for copy in first:
        copy.start()

    def rows_of(b, c):
        return wbuf.at[b, pl.ds(pl.multiple_of(parity * half + c * piece, piece), piece)]

    def along(b, c, up):
        return remote(
            rows_of(b, c), rows_of(b, c), w_send.at[up, b, c], w_recv.at[b, c],
            {"sp": z + 1 if up else z - 1},
        )

    def across(b, c):
        return remote(rows_of(b, c), rows_of(b, c), y_send.at[b, c], y_recv.at[b, c], {"grp": partner})

    has_up, has_down = z < n_sp - 1, z > 0
    reach = n_sp - 2
    at_edge = jnp.logical_or(z == 0, z == n_sp - 1)
    far = jnp.where(z == 0, n_sp - 1, 0)
    ask = remote(gall.at[far, :, pl.ds(0, cols)], far_gained, f_send.at[0], f_recv.at[0], {"sp": far})
    answer = remote(far_out, far_in, f_send.at[1], f_recv.at[1], {"sp": far})
    loads[2].wait()
    for c in range(CHUNKS):
        @pl.when(has_up)
        def _():
            along(z, c, 1).start()

        @pl.when(has_down)
        def _():
            along(z, c, 0).start()

    def event(k, c):
        @pl.when(z >= k)
        def _():
            b = z - k
            along(b, c, 1).wait_recv()

            if k < reach:
                @pl.when(has_up)
                def _():
                    along(b, c, 1).start()

            across(b, c).start()

        @pl.when(z + k < n_sp)
        def _():
            b = z + k
            along(b, c, 0).wait_recv()

            if k < reach:
                @pl.when(has_down)
                def _():
                    along(b, c, 0).start()

            across(b, c).start()

    def block_product(b):
        acc[...] += jnp.dot(gall[b, :, :cols], wbuf[b], preferred_element_type=jnp.float32)

    def finish(k):
        @pl.when(z >= k)
        def _():
            for c in range(CHUNKS):
                across(z - k, c).wait_recv()
            block_product(z - k)

        @pl.when(z + k < n_sp)
        def _():
            for c in range(CHUNKS):
                across(z + k, c).wait_recv()
            block_product(z + k)

    second = []
    for d in range(1, n_tp):
        target = {"tp": lax.rem(t + d, n_tp)}
        second.append(remote(lat.at[:, t], lat.at[:, t], s2_send.at[0, d], s2_recv.at[0, d], target))
        second.append(remote(rot.at[:, t], rot.at[:, t], s2_send.at[1, d], s2_recv.at[1, d], target))

    def queries():
        loads[3].wait()
        loads[4].wait()
        loads[5].wait()
        wide = ql[...].astype(jnp.float32)
        mean = jnp.mean(wide * wide, axis=-1, keepdims=True)
        gain = jnp.concatenate([qg[i : i + 1] for i in range(qg.shape[0])], axis=1)
        qnorm[...] = (wide * lax.rsqrt(mean + norm_eps) * gain).astype(jnp.bfloat16)
        qfull[...] = jnp.dot(qnorm[...], qbuf[...], preferred_element_type=jnp.float32).astype(
            jnp.bfloat16
        )

    def spread():
        for copy in first:
            copy.wait_recv()
        for copy in second:
            copy.start()

    def latents():
        for load in loads[6:11]:
            load.wait()
        for copy in second:
            copy.wait_recv()
        wide = lat[...].reshape(keys, lat.shape[-1]).astype(jnp.float32)
        mean = jnp.mean(wide * wide, axis=-1, keepdims=True)
        latn[...] = (wide * lax.rsqrt(mean + norm_eps) * lg[...]).astype(jnp.bfloat16)
        spun = rot[...].reshape(keys, rot.shape[-1]).astype(jnp.float32)
        kturn[...] = turned(spun, table[...]).astype(jnp.bfloat16)

    transposed = (((1,), (1,)), ((), ()))

    def attend(h):
        start = h * head_width
        plain = qfull[:, start : start + NOPE_DIM]
        spun = qfull[:, start + NOPE_DIM : start + head_width].astype(jnp.float32)
        own = table[pl.ds(pl.multiple_of(z * block_rows, block_rows), block_rows), :]
        spun = turned(spun, own).astype(jnp.bfloat16)
        key_plain = jnp.dot(
            latn[...], kbuf[:, h * NOPE_DIM : (h + 1) * NOPE_DIM], preferred_element_type=jnp.float32
        ).astype(jnp.bfloat16)
        scores = lax.dot_general(plain, key_plain, transposed, preferred_element_type=jnp.float32)
        scores = scores + lax.dot_general(
            spun, kturn[...], transposed, preferred_element_type=jnp.float32
        )
        scores = scores * (head_width ** (-0.5))
        expo = jnp.exp(scores - jnp.max(scores, axis=-1, keepdims=True))
        total = jnp.sum(expo, axis=-1, keepdims=True)
        mix = jnp.dot(expo.astype(jnp.bfloat16), latn[...], preferred_element_type=jnp.float32)
        mix = (mix / total).astype(jnp.bfloat16)
        head_out = jnp.dot(
            mix, vbuf[:, h * VALUE_DIM : (h + 1) * VALUE_DIM], preferred_element_type=jnp.float32
        ).astype(jnp.bfloat16)
        wide = head_out.astype(jnp.float32)
        gained = wide * og[:, h * VALUE_DIM : (h + 1) * VALUE_DIM]
        gall[t, :, h * VALUE_DIM : (h + 1) * VALUE_DIM] = gained.astype(jnp.bfloat16)
        square = jnp.sum(wide * wide, axis=-1, keepdims=True)
        if h:
            square = square + acc[:, :1]
        acc[:, :VALUE_DIM] = jnp.broadcast_to(square, (block_rows, VALUE_DIM))
        if h == heads - 1:
            gall[t, :, cols:] = acc[:, :VALUE_DIM].astype(jnp.bfloat16)

    def head_part(h):
        width = VALUE_DIM if h < heads - 1 else 2 * VALUE_DIM
        return gall.at[t, :, pl.ds(h * VALUE_DIM, width)]

    shares = [
        [
            remote(head_part(h), head_part(h), g_send.at[h, d], g_recv.at[h, d], {"tp": lax.rem(t + d, n_tp)})
            for d in range(1, n_tp)
        ]
        for h in range(heads)
    ]

    def share(h):
        for copy in shares[h]:
            copy.start()

    def far_ask():
        for copy in sum(shares, []):
            copy.wait_recv()

        @pl.when(at_edge)
        def _():
            ask.start()

    def far_product():
        loads[11].wait()

        @pl.when(at_edge)
        def _():
            ask.wait_recv()
            far_out[...] = jnp.dot(
                far_gained[...], wbuf[z], preferred_element_type=jnp.float32
            ).astype(jnp.bfloat16)

    def own_product():
        acc[...] = jnp.zeros_like(acc)
        block_product(z)

    def far_answer():
        @pl.when(at_edge)
        def _():
            answer.start()

    work = [functools.partial(attend, h) for h in range(heads)]
    sends = [functools.partial(share, h) for h in range(heads)]
    middle = (heads + 1) // 2
    early = [call for pair in zip(work[:middle], [None] + sends[: middle - 1]) for call in pair if call]
    late = [
        call
        for pair in zip(work[middle:], sends[middle - 1 : heads - 1])
        for call in pair
    ]
    tasks = {
        0: [queries, spread],
        1: [latents] + early,
        2: late,
        3: sends[heads - 1 :],
        4: [far_ask],
        6: [far_product, own_product, far_answer],
    }
    slot = 0
    for k in range(1, reach + 1):
        for c in range(CHUNKS):
            for task in tasks.pop(slot, []):
                task()
            event(k, c)
            slot += 1
    for left in sorted(tasks):
        for task in tasks[left]:
            task()
    for k in range(1, reach + 1):
        finish(k)

    @pl.when(at_edge)
    def _():
        answer.wait_recv()
        acc[...] += far_in[...].astype(jnp.float32)

    squares = gall[0, :, cols : cols + 1].astype(jnp.float32)
    for p in range(1, n_tp):
        squares = squares + gall[p, :, cols : cols + 1].astype(jnp.float32)
    scale = lax.rsqrt(squares / (n_tp * cols) + norm_eps)
    out[...] = (acc[...] * scale).astype(out.dtype)

    for copy in first + second + sum(shares, []):
        copy.wait_send()
    for c in range(CHUNKS):
        @pl.when(has_up)
        def _():
            along(z, c, 1).wait_send()

        @pl.when(has_down)
        def _():
            along(z, c, 0).wait_send()

    @pl.when(at_edge)
    def _():
        ask.wait_send()
        answer.wait_send()

    for k in range(1, reach + 1):
        for c in range(CHUNKS):
            @pl.when(z >= k)
            def _():
                across(z - k, c).wait_send()

            @pl.when(z + k < n_sp)
            def _():
                across(z + k, c).wait_send()

            if k < reach:
                @pl.when(jnp.logical_and(z >= k, has_up))
                def _():
                    along(z - k, c, 1).wait_send()

                @pl.when(jnp.logical_and(z + k < n_sp, has_down))
                def _():
                    along(z + k, c, 0).wait_send()


MESH = pl.DeviceIdType.MESH


def on_device_fused(
    n_sp, n_tp,
    query_latent, key_latent, rotary_key, query_gain, latent_gain,
    query_up, key_up, value_up, out_gain, out_weight,
):
    block_rows, row_count = query_latent.shape[0], key_latent.shape[0]
    rank, width = key_latent.shape[1], rotary_key.shape[1]
    keys = n_sp * n_tp * row_count
    depth, features = out_weight.shape
    cols = value_up.shape[1]
    vmem, bf16, dma = pltpu.VMEM, jnp.bfloat16, pltpu.SemaphoreType.DMA
    table = jnp.asarray(rope_table(keys, width))
    in_vmem = pl.BlockSpec(memory_space=pltpu.VMEM)
    in_hbm = pl.BlockSpec(memory_space=pl.ANY)
    return pl.pallas_call(
        functools.partial(kernel, n_sp, n_tp),
        out_shape=jax.ShapeDtypeStruct((block_rows, features), bf16),
        in_specs=[in_hbm] * 11,
        out_specs=in_vmem,
        scratch_shapes=[
            vmem(query_latent.shape, bf16),
            vmem((query_gain.shape[0] // LANES, LANES), jnp.float32),
            vmem((1, rank), jnp.float32),
            vmem((1, cols), jnp.float32),
            vmem(table.shape, jnp.float32),
            vmem((n_sp, n_tp, row_count, rank), bf16),
            vmem((n_sp, n_tp, row_count, width), bf16),
            vmem((n_sp, depth, features), bf16),
            vmem(query_up.shape, bf16),
            vmem(key_up.shape, bf16),
            vmem(value_up.shape, bf16),
            vmem((keys, rank), bf16),
            vmem((keys, width), bf16),
            vmem((block_rows, query_up.shape[1]), bf16),
            vmem(query_latent.shape, bf16),
            vmem((n_tp, block_rows, cols + VALUE_DIM), bf16),
            vmem((block_rows, features), jnp.float32),
            vmem((block_rows, cols), bf16),
            vmem((block_rows, features), bf16),
            vmem((block_rows, features), bf16),
            dma((12,)),
            dma((2, n_sp)),
            dma((2, n_sp)),
            dma((2, n_tp)),
            dma((2, n_tp)),
            dma((cols // VALUE_DIM, n_tp)),
            dma((cols // VALUE_DIM, n_tp)),
            dma((2, n_sp, CHUNKS)),
            dma((n_sp, CHUNKS)),
            dma((n_sp, CHUNKS)),
            dma((n_sp, CHUNKS)),
            dma((2,)),
            dma((2,)),
        ],
        compiler_params=pltpu.CompilerParams(
            collective_id=0, has_side_effects=True
        ),
    )(
        query_latent, key_latent, rotary_key, query_gain.reshape(-1, LANES), latent_gain[None], out_gain[None],
        table, query_up, key_up, value_up, out_weight,
    )


def fits_fused(mesh):
    n_grp, n_sp, n_tp = (mesh.shape[name] for name in ("grp", "sp", "tp"))
    return n_grp % 2 == 0 and 2 < n_sp <= MOST_STEPS and n_sp == n_tp


def solution(mesh):
    in_specs = (
        P(("grp", "sp"), None),
        P(("grp", "sp", "tp"), None),
        P(("grp", "sp", "tp"), None),
        P(),
        P(),
        P(None, "tp"),
        P(None, "tp"),
        P(None, "tp"),
        P("tp"),
        P("sp", "tp"),
    )
    out_specs = P(("grp", "sp"), "tp")
    step = on_device
    if fits_fused(mesh):
        step = functools.partial(on_device_fused, mesh.shape["sp"], mesh.shape["tp"])
    return jax.shard_map(
        step, mesh=mesh, in_specs=in_specs, out_specs=out_specs, check_vma=False
    )
```

```python
import functools

import jax
import jax.numpy as jnp
import numpy as np
from jax import lax
from jax.experimental import pallas as pl
from jax.experimental.pallas import tpu as pltpu
from jax.sharding import PartitionSpec as P

HEADS = 16
NOPE_DIM = 128
ROPE_DIM = 64
VALUE_DIM = 128
KVRANK = 256


norm_eps = 1e-06
rope_theta = 10000.0


def rms_scaled(inputs, gain_vec):
    widened = inputs.astype(jnp.float32)
    return (
        widened
        * lax.rsqrt(jnp.mean(widened * widened, axis=-1, keepdims=True) + norm_eps)
        * gain_vec
    )


def rotate_half(inputs, positions):
    half_width = inputs.shape[-1] // 2
    inverse = rope_theta ** (-jnp.arange(half_width, dtype=jnp.float32) / half_width)
    angles = positions[:, None] * inverse[None, :]
    if inputs.ndim == 3:
        angles = angles[:, None, :]
    cosine = jnp.cos(angles)
    sine = jnp.sin(angles)
    widened = inputs.astype(jnp.float32)
    first = widened[..., :half_width]
    second = widened[..., half_width:]
    return jnp.concatenate(
        [first * cosine - second * sine, second * cosine + first * sine], axis=-1
    )


def on_device(
    query_latent,
    key_latent,
    rotary_key,
    query_gain,
    latent_gain,
    query_up,
    key_up,
    value_up,
    out_gain,
    out_weight,
):
    block_rows = query_latent.shape[0]
    row_count = key_latent.shape[0]
    head_local = key_up.shape[1] // NOPE_DIM
    block_start = lax.axis_index("sp") * block_rows
    own_start = block_start + lax.axis_index("tp") * row_count
    score_scale = (NOPE_DIM + ROPE_DIM) ** (-0.5)
    normed = rms_scaled(query_latent, query_gain).astype(jnp.bfloat16)
    query_full = jnp.dot(normed, query_up, preferred_element_type=jnp.float32).astype(jnp.bfloat16)
    query_full = query_full.reshape(block_rows, head_local, NOPE_DIM + ROPE_DIM)
    query_positions = (block_start + jnp.arange(block_rows, dtype=jnp.int32)).astype(jnp.float32)
    query_plain = query_full[..., :NOPE_DIM]
    query_turned = rotate_half(query_full[..., NOPE_DIM:], query_positions).astype(jnp.bfloat16)
    latent_normed = rms_scaled(key_latent, latent_gain).astype(jnp.bfloat16)
    own_positions = (own_start + jnp.arange(row_count, dtype=jnp.int32)).astype(jnp.float32)
    key_turned = rotate_half(rotary_key, own_positions).astype(jnp.bfloat16)
    running_max = jnp.full((block_rows, head_local), -1e30, jnp.float32)
    running_sum = jnp.zeros((block_rows, head_local), jnp.float32)
    weighted = jnp.zeros((block_rows, head_local, KVRANK), jnp.float32)
    latents = lax.all_gather(latent_normed, ("sp", "tp"), axis=0, tiled=True)
    turned_keys = lax.all_gather(key_turned, ("sp", "tp"), axis=0, tiled=True)
    portion_rows = latents.shape[0]
    step_rows = min(portion_rows, 2048)
    for begin in range(0, portion_rows, step_rows):
        latent_part = latents[begin : begin + step_rows]
        turned_part = turned_keys[begin : begin + step_rows]
        key_plain = jnp.dot(latent_part, key_up, preferred_element_type=jnp.float32).astype(
            jnp.bfloat16
        )
        key_plain = key_plain.reshape(latent_part.shape[0], head_local, NOPE_DIM)
        scores = jnp.einsum(
            "qhd,khd->qhk", query_plain, key_plain, preferred_element_type=jnp.float32
        )
        scores = scores + jnp.einsum(
            "qhd,kd->qhk", query_turned, turned_part, preferred_element_type=jnp.float32
        )
        scores = scores * score_scale
        new_max = jnp.maximum(running_max, jnp.max(scores, axis=-1))
        rescale = jnp.exp(running_max - new_max)
        expo = jnp.exp(scores - new_max[..., None])
        running_sum = running_sum * rescale + jnp.sum(expo, axis=-1)
        weighted = weighted * rescale[..., None] + jnp.einsum(
            "qhk,kc->qhc",
            expo.astype(jnp.bfloat16),
            latent_part,
            preferred_element_type=jnp.float32,
        )
        running_max = new_max
    final_state = (running_max, running_sum, weighted)
    running_max, running_sum, weighted = final_state
    latent_mix = (weighted / running_sum[..., None]).astype(jnp.bfloat16)
    value_heads = value_up.reshape(KVRANK, head_local, VALUE_DIM)
    head_out = jnp.einsum(
        "qhc,chd->qhd", latent_mix, value_heads, preferred_element_type=jnp.float32
    ).astype(jnp.bfloat16)
    head_out = head_out.reshape(block_rows, head_local * VALUE_DIM)
    widened = head_out.astype(jnp.float32)
    square_part = jnp.sum(widened * widened, axis=1)
    gained = (widened * out_gain).astype(jnp.bfloat16)
    all_gained, square_parts = (
        lax.all_gather(gained, "tp", axis=1, tiled=True),
        lax.all_gather(square_part[:, None].astype(jnp.bfloat16), "tp", axis=1, tiled=True).astype(
            jnp.float32
        ),
    )
    all_squares = jnp.sum(square_parts, axis=1)
    own_sums = jnp.dot(
        all_gained,
        lax.all_gather(out_weight, "sp", axis=0, tiled=True),
        preferred_element_type=jnp.float32,
    )
    mean_square = all_squares / (HEADS * VALUE_DIM)
    return (own_sums * lax.rsqrt(mean_square + norm_eps)[:, None]).astype(jnp.bfloat16)


CHUNKS = 4
LANES = 128
MOST_STEPS = 8


def rope_table(tokens, width):
    half = width // 2
    inverse = np.float32(rope_theta) ** (-np.arange(half, dtype=np.float32) / np.float32(half))
    angles = np.arange(tokens, dtype=np.float32)[:, None] * inverse.astype(np.float32)[None, :]
    wide = angles.astype(np.float32).astype(np.float64)
    cosine, sine = np.cos(wide), np.sin(wide)
    return np.concatenate([cosine, cosine, -sine, sine], axis=1).astype(np.float32)


def turned(wide, table):
    width = wide.shape[-1]
    half = width // 2
    swapped = jnp.concatenate([wide[:, half:], wide[:, :half]], axis=1)
    return wide * table[:, :width] + swapped * table[:, width:]


def kernel(
    n_sp, n_tp,
    ql_hbm, kl, rk, qg_hbm, lg_hbm, og_hbm, table_hbm, qup, kup, vup, ow, out,
    ql, qg, lg, og, table,
    lat, rot, wbuf, qbuf, kbuf, vbuf, latn, kturn, qfull, qnorm, gall, acc,
    far_gained, far_out, far_in,
    local, s1_send, s1_recv, s2_send, s2_recv, g_send, g_recv,
    w_send, w_recv, y_send, y_recv, f_send, f_recv,
):
    z, t, g = lax.axis_index("sp"), lax.axis_index("tp"), lax.axis_index("grp")
    parity = lax.rem(g, 2)
    partner = g + 1 - 2 * parity
    block_rows = ql.shape[0]
    depth = ow.shape[0]
    half = depth // 2
    piece = half // CHUNKS
    heads = kup.shape[1] // NOPE_DIM
    cols = heads * VALUE_DIM
    head_width = NOPE_DIM + ROPE_DIM
    keys = n_sp * n_tp * kl.shape[0]

    near = pl.ds(pl.multiple_of(parity * half, half), half)
    far_half = pl.ds(pl.multiple_of((1 - parity) * half, half), half)
    loads = [
        pltpu.make_async_copy(src, dst, local.at[i])
        for i, (src, dst) in enumerate((
            (kl, lat.at[z, t]),
            (rk, rot.at[z, t]),
            (ow.at[near], wbuf.at[z, near]),
            (ql_hbm, ql),
            (qg_hbm, qg),
            (qup, qbuf),
            (lg_hbm, lg),
            (table_hbm, table),
            (kup, kbuf),
            (vup, vbuf),
            (og_hbm, og),
            (ow.at[far_half], wbuf.at[z, far_half]),
        ))
    ]
    for load in loads:
        load.start()

    barrier = pltpu.get_barrier_semaphore()
    for d in range(1, n_sp):
        pl.semaphore_signal(barrier, inc=1, device_id={"sp": lax.rem(z + d, n_sp)}, device_id_type=MESH)
    for d in range(1, n_tp):
        pl.semaphore_signal(barrier, inc=1, device_id={"tp": lax.rem(t + d, n_tp)}, device_id_type=MESH)
    pl.semaphore_signal(barrier, inc=1, device_id={"grp": partner}, device_id_type=MESH)
    pl.semaphore_wait(barrier, n_sp + n_tp - 1)

    def remote(src, dst, send, recv, target):
        return pltpu.make_async_remote_copy(
            src_ref=src, dst_ref=dst, send_sem=send, recv_sem=recv,
            device_id=target, device_id_type=MESH,
        )

    first = []
    for d in range(1, n_sp):
        target = {"sp": lax.rem(z + d, n_sp)}
        first.append(remote(lat.at[z, t], lat.at[z, t], s1_send.at[0, d], s1_recv.at[0, d], target))
        first.append(remote(rot.at[z, t], rot.at[z, t], s1_send.at[1, d], s1_recv.at[1, d], target))
    loads[0].wait()
    loads[1].wait()
    for copy in first:
        copy.start()

    def rows_of(b, c):
        return wbuf.at[b, pl.ds(pl.multiple_of(parity * half + c * piece, piece), piece)]

    def along(b, c, up):
        return remote(
            rows_of(b, c), rows_of(b, c), w_send.at[up, b, c], w_recv.at[b, c],
            {"sp": z + 1 if up else z - 1},
        )

    def far_rows_of(b, c):
        return wbuf.at[b, pl.ds(pl.multiple_of((1 - parity) * half + c * piece, piece), piece)]

    def along_far(c):
        return remote(
            far_rows_of(z, c), far_rows_of(z, c), y_send.at[z, c], y_recv.at[z, c],
            {"sp": jnp.where(z == 0, 1, n_sp - 2)},
        )

    def across(b, c):
        return remote(rows_of(b, c), rows_of(b, c), y_send.at[b, c], y_recv.at[b, c], {"grp": partner})

    has_up, has_down = z < n_sp - 1, z > 0
    reach = n_sp - 2
    at_edge = jnp.logical_or(z == 0, z == n_sp - 1)
    far = jnp.where(z == 0, n_sp - 1, 0)
    ask = remote(gall.at[far, :, pl.ds(0, cols)], far_gained, f_send.at[0], f_recv.at[0], {"sp": far})
    answer = remote(far_out, far_in, f_send.at[1], f_recv.at[1], {"sp": far})
    loads[2].wait()
    for c in range(CHUNKS):
        @pl.when(has_up)
        def _():
            along(z, c, 1).start()

        @pl.when(has_down)
        def _():
            along(z, c, 0).start()

    def event(k, c):
        @pl.when(z >= k)
        def _():
            b = z - k
            along(b, c, 1).wait_recv()

            if k < reach:
                @pl.when(has_up)
                def _():
                    along(b, c, 1).start()

            if k == 1:
                @pl.when(z > 1)
                def _():
                    across(b, c).start()
            else:
                across(b, c).start()

        @pl.when(z + k < n_sp)
        def _():
            b = z + k
            along(b, c, 0).wait_recv()

            if k < reach:
                @pl.when(has_down)
                def _():
                    along(b, c, 0).start()

            if k == 1:
                @pl.when(z < n_sp - 2)
                def _():
                    across(b, c).start()
            else:
                across(b, c).start()

    def block_product(b):
        acc[...] += jnp.dot(gall[b, :, :cols], wbuf[b], preferred_element_type=jnp.float32)

    def finish(k):
        @pl.when(z >= k)
        def _():
            for c in range(CHUNKS):
                across(z - k, c).wait_recv()
            block_product(z - k)

        @pl.when(z + k < n_sp)
        def _():
            for c in range(CHUNKS):
                across(z + k, c).wait_recv()
            block_product(z + k)

    second = []
    for d in range(1, n_tp):
        target = {"tp": lax.rem(t + d, n_tp)}
        second.append(remote(lat.at[:, t], lat.at[:, t], s2_send.at[0, d], s2_recv.at[0, d], target))
        second.append(remote(rot.at[:, t], rot.at[:, t], s2_send.at[1, d], s2_recv.at[1, d], target))

    def queries():
        loads[3].wait()
        loads[4].wait()
        loads[5].wait()
        wide = ql[...].astype(jnp.float32)
        mean = jnp.mean(wide * wide, axis=-1, keepdims=True)
        gain = jnp.concatenate([qg[i : i + 1] for i in range(qg.shape[0])], axis=1)
        qnorm[...] = (wide * lax.rsqrt(mean + norm_eps) * gain).astype(jnp.bfloat16)
        qfull[...] = jnp.dot(qnorm[...], qbuf[...], preferred_element_type=jnp.float32).astype(
            jnp.bfloat16
        )

    def far_halves():
        loads[11].wait()

        @pl.when(at_edge)
        def _():
            for c in range(CHUNKS):
                along_far(c).start()

    def spread():
        for copy in first:
            copy.wait_recv()
        for copy in second:
            copy.start()

    def latents():
        for load in loads[6:11]:
            load.wait()
        for copy in second:
            copy.wait_recv()
        wide = lat[...].reshape(keys, lat.shape[-1]).astype(jnp.float32)
        mean = jnp.mean(wide * wide, axis=-1, keepdims=True)
        latn[...] = (wide * lax.rsqrt(mean + norm_eps) * lg[...]).astype(jnp.bfloat16)
        spun = rot[...].reshape(keys, rot.shape[-1]).astype(jnp.float32)
        kturn[...] = turned(spun, table[...]).astype(jnp.bfloat16)

    transposed = (((1,), (1,)), ((), ()))

    def attend(h):
        start = h * head_width
        plain = qfull[:, start : start + NOPE_DIM]
        spun = qfull[:, start + NOPE_DIM : start + head_width].astype(jnp.float32)
        own = table[pl.ds(pl.multiple_of(z * block_rows, block_rows), block_rows), :]
        spun = turned(spun, own).astype(jnp.bfloat16)
        key_plain = jnp.dot(
            latn[...], kbuf[:, h * NOPE_DIM : (h + 1) * NOPE_DIM], preferred_element_type=jnp.float32
        ).astype(jnp.bfloat16)
        scores = lax.dot_general(plain, key_plain, transposed, preferred_element_type=jnp.float32)
        scores = scores + lax.dot_general(
            spun, kturn[...], transposed, preferred_element_type=jnp.float32
        )
        scores = scores * (head_width ** (-0.5))
        expo = jnp.exp(scores - jnp.max(scores, axis=-1, keepdims=True))
        total = jnp.sum(expo, axis=-1, keepdims=True)
        mix = jnp.dot(expo.astype(jnp.bfloat16), latn[...], preferred_element_type=jnp.float32)
        mix = (mix / total).astype(jnp.bfloat16)
        head_out = jnp.dot(
            mix, vbuf[:, h * VALUE_DIM : (h + 1) * VALUE_DIM], preferred_element_type=jnp.float32
        ).astype(jnp.bfloat16)
        wide = head_out.astype(jnp.float32)
        gained = wide * og[:, h * VALUE_DIM : (h + 1) * VALUE_DIM]
        gall[t, :, h * VALUE_DIM : (h + 1) * VALUE_DIM] = gained.astype(jnp.bfloat16)
        square = jnp.sum(wide * wide, axis=-1, keepdims=True)
        if h:
            square = square + acc[:, :1]
        acc[:, :VALUE_DIM] = jnp.broadcast_to(square, (block_rows, VALUE_DIM))
        if h == heads - 1:
            gall[t, :, cols:] = acc[:, :VALUE_DIM].astype(jnp.bfloat16)

    def head_part(h):
        width = VALUE_DIM if h < heads - 1 else 2 * VALUE_DIM
        return gall.at[t, :, pl.ds(h * VALUE_DIM, width)]

    shares = [
        [
            remote(head_part(h), head_part(h), g_send.at[h, d], g_recv.at[h, d], {"tp": lax.rem(t + d, n_tp)})
            for d in range(1, n_tp)
        ]
        for h in range(heads)
    ]

    def share(h):
        for copy in shares[h]:
            copy.start()

    def far_ask():
        for copy in sum(shares, []):
            copy.wait_recv()

        @pl.when(at_edge)
        def _():
            ask.start()

    def far_product():
        @pl.when(at_edge)
        def _():
            ask.wait_recv()
            far_out[...] = jnp.dot(
                far_gained[...], wbuf[z], preferred_element_type=jnp.float32
            ).astype(jnp.bfloat16)

    def own_product():
        acc[...] = jnp.zeros_like(acc)
        block_product(z)

    def far_answer():
        @pl.when(at_edge)
        def _():
            answer.start()

    work = [functools.partial(attend, h) for h in range(heads)]
    sends = [functools.partial(share, h) for h in range(heads)]
    middle = (heads + 1) // 2
    early = [call for pair in zip(work[:middle], [None] + sends[: middle - 1]) for call in pair if call]
    late = [
        call
        for pair in zip(work[middle:], sends[middle - 1 : heads - 1])
        for call in pair
    ]
    tasks = {
        0: [queries, far_halves, spread],
        1: [latents] + early,
        2: late,
        3: sends[heads - 1 :],
        4: [far_ask],
        7: [far_product, own_product, far_answer],
    }
    slot = 0
    for k in range(1, reach + 1):
        for c in range(CHUNKS):
            for task in tasks.pop(slot, []):
                task()
            event(k, c)
            slot += 1
    for left in sorted(tasks):
        for task in tasks[left]:
            task()
    for k in range(1, reach + 1):
        finish(k)

    @pl.when(at_edge)
    def _():
        answer.wait_recv()
        acc[...] += far_in[...].astype(jnp.float32)

    squares = gall[0, :, cols : cols + 1].astype(jnp.float32)
    for p in range(1, n_tp):
        squares = squares + gall[p, :, cols : cols + 1].astype(jnp.float32)
    scale = lax.rsqrt(squares / (n_tp * cols) + norm_eps)
    out[...] = (acc[...] * scale).astype(out.dtype)

    for copy in first + second + sum(shares, []):
        copy.wait_send()
    for c in range(CHUNKS):
        @pl.when(has_up)
        def _():
            along(z, c, 1).wait_send()

        @pl.when(has_down)
        def _():
            along(z, c, 0).wait_send()

    @pl.when(at_edge)
    def _():
        ask.wait_send()
        answer.wait_send()
        for c in range(CHUNKS):
            along_far(c).wait_send()

    for k in range(1, reach + 1):
        for c in range(CHUNKS):
            @pl.when(z >= max(k, 2))
            def _():
                across(z - k, c).wait_send()

            @pl.when(z + max(k, 2) < n_sp)
            def _():
                across(z + k, c).wait_send()

            if k < reach:
                @pl.when(jnp.logical_and(z >= k, has_up))
                def _():
                    along(z - k, c, 1).wait_send()

                @pl.when(jnp.logical_and(z + k < n_sp, has_down))
                def _():
                    along(z + k, c, 0).wait_send()


MESH = pl.DeviceIdType.MESH


def on_device_fused(
    n_sp, n_tp,
    query_latent, key_latent, rotary_key, query_gain, latent_gain,
    query_up, key_up, value_up, out_gain, out_weight,
):
    block_rows, row_count = query_latent.shape[0], key_latent.shape[0]
    rank, width = key_latent.shape[1], rotary_key.shape[1]
    keys = n_sp * n_tp * row_count
    depth, features = out_weight.shape
    cols = value_up.shape[1]
    vmem, bf16, dma = pltpu.VMEM, jnp.bfloat16, pltpu.SemaphoreType.DMA
    table = jnp.asarray(rope_table(keys, width))
    in_vmem = pl.BlockSpec(memory_space=pltpu.VMEM)
    in_hbm = pl.BlockSpec(memory_space=pl.ANY)
    return pl.pallas_call(
        functools.partial(kernel, n_sp, n_tp),
        out_shape=jax.ShapeDtypeStruct((block_rows, features), bf16),
        in_specs=[in_hbm] * 11,
        out_specs=in_vmem,
        scratch_shapes=[
            vmem(query_latent.shape, bf16),
            vmem((query_gain.shape[0] // LANES, LANES), jnp.float32),
            vmem((1, rank), jnp.float32),
            vmem((1, cols), jnp.float32),
            vmem(table.shape, jnp.float32),
            vmem((n_sp, n_tp, row_count, rank), bf16),
            vmem((n_sp, n_tp, row_count, width), bf16),
            vmem((n_sp, depth, features), bf16),
            vmem(query_up.shape, bf16),
            vmem(key_up.shape, bf16),
            vmem(value_up.shape, bf16),
            vmem((keys, rank), bf16),
            vmem((keys, width), bf16),
            vmem((block_rows, query_up.shape[1]), bf16),
            vmem(query_latent.shape, bf16),
            vmem((n_tp, block_rows, cols + VALUE_DIM), bf16),
            vmem((block_rows, features), jnp.float32),
            vmem((block_rows, cols), bf16),
            vmem((block_rows, features), bf16),
            vmem((block_rows, features), bf16),
            dma((12,)),
            dma((2, n_sp)),
            dma((2, n_sp)),
            dma((2, n_tp)),
            dma((2, n_tp)),
            dma((cols // VALUE_DIM, n_tp)),
            dma((cols // VALUE_DIM, n_tp)),
            dma((2, n_sp, CHUNKS)),
            dma((n_sp, CHUNKS)),
            dma((n_sp, CHUNKS)),
            dma((n_sp, CHUNKS)),
            dma((2,)),
            dma((2,)),
        ],
        compiler_params=pltpu.CompilerParams(
            collective_id=0, has_side_effects=True
        ),
    )(
        query_latent, key_latent, rotary_key, query_gain.reshape(-1, LANES), latent_gain[None], out_gain[None],
        table, query_up, key_up, value_up, out_weight,
    )


def fits_fused(mesh):
    n_grp, n_sp, n_tp = (mesh.shape[name] for name in ("grp", "sp", "tp"))
    return n_grp % 2 == 0 and 2 < n_sp <= MOST_STEPS and n_sp == n_tp


def solution(mesh):
    in_specs = (
        P(("grp", "sp"), None),
        P(("grp", "sp", "tp"), None),
        P(("grp", "sp", "tp"), None),
        P(),
        P(),
        P(None, "tp"),
        P(None, "tp"),
        P(None, "tp"),
        P("tp"),
        P("sp", "tp"),
    )
    out_specs = P(("grp", "sp"), "tp")
    step = on_device
    if fits_fused(mesh):
        step = functools.partial(on_device_fused, mesh.shape["sp"], mesh.shape["tp"])
    return jax.shard_map(
        step, mesh=mesh, in_specs=in_specs, out_specs=out_specs, check_vma=False
    )
```
